32 devices in a mesh: fs: 8 (over z, y), tp: 4 (over x, core).
Axes of the slice: x: 2, y: 2, z: 4, core: 2. Of those that a mesh axis runs over, the one named last changes fastest.
Arguments:
- tokens: bfloat16 [640, 3072], P('tp'), may hold values from -6 to 6
- gain_first: float32 [3072], replicated, may hold values from 0.1 to 1.9
- gain_second: float32 [3072], replicated, may hold values from 0.1 to 1.9
- gate_first: float32 [3072, 8192], P('fs', 'tp'), may hold values from -0.109375 to 0.109375
- up_first: float32 [3072, 8192], P('fs', 'tp'), may hold values from -0.109375 to 0.109375
- down_first: float32 [8192, 3072], P('fs', 'tp'), may hold values from -0.09375 to 0.09375
- gate_second: float32 [3072, 8192], P('fs', 'tp'), may hold values from -0.109375 to 0.109375
- up_second: float32 [3072, 8192], P('fs', 'tp'), may hold values from -0.109375 to 0.109375
- down_second: float32 [8192, 3072], P('fs', 'tp'), may hold values from -0.09375 to 0.09375
Outputs:
- result_rows: bfloat16 [640, 3072], P('tp')
- serve_gate_first: bfloat16 [3072, 8192], P(None, 'fs')
- serve_up_first: bfloat16 [3072, 8192], P(None, 'fs')
- serve_down_first: bfloat16 [8192, 3072], P('fs')
- serve_gate_second: bfloat16 [3072, 8192], P(None, 'fs')
- serve_up_second: bfloat16 [3072, 8192], P(None, 'fs')
- serve_down_second: bfloat16 [8192, 3072], P('fs')
The draws below stay inside these ranges and needn't reach their ends.
All inputs are finite; a program needn't handle non-finite values.
Results may differ from the reference program's by a relative error of at most 0.011.
Values may be sent and summed in bfloat16 or wider, within the bound.
A program may use at most 192 MiB of HBM per device.

```python
import jax
import jax.numpy as jnp
from jax import lax

D = 3072
FF = 8192
TOKENS = 640


def with_spikes(drawn, own_key, source, target, shards_of, factor):
    def block_of(axis_at):
        return (jnp.arange(drawn.shape[axis_at]) // (drawn.shape[axis_at] // shards_of)).reshape((-1,) + (1,) * (drawn.ndim - 1 - axis_at))

    first = jax.random.permutation(own_key, shards_of)[block_of(target)]
    far = (block_of(target) + shards_of // 2) % shards_of
    return jnp.where((block_of(source) == first) | (block_of(source) == far), factor * drawn, drawn)


def level_of(stream_key, dims, split, smallest, largest):
    def one(dim, parts):
        draws = jax.random.uniform(jax.random.fold_in(jax.random.fold_in(stream_key, 6), dim), (parts,), jnp.float32, smallest / len(split), largest / len(split))
        return jnp.repeat(jnp.exp(draws), dims[dim] // parts).reshape((-1,) + (1,) * (len(dims) - dim - 1))

    level = one(*split[0])
    for cut in split[1:]:
        level = level * one(*cut)
    return level


def scatter_about(key, extent, deviation, most, shards=(), held_as=jnp.bfloat16):
    values = deviation * jax.random.normal(key, extent, jnp.float32)
    if shards:
        values = values * level_of(key, extent, shards, -0.22, 0.18)
    return jnp.clip(values, -most, most).astype(held_as)


def bell_draw_with(stream_key, dims, width, most, shards, heavy, kind=jnp.bfloat16):
    array = width * jax.random.normal(stream_key, dims, jnp.float32)
    if shards:
        array = array * level_of(stream_key, dims, shards, -0.22, 0.18)
    return jnp.clip(with_spikes(array, jax.random.fold_in(stream_key, 3), *heavy), -most, most).astype(kind)


def setup_inputs(seed: int = 0) -> dict:
    seeds = jax.random.split(jax.random.key(seed), 10)
    tokens = scatter_about(seeds[0], (TOKENS, D), 1.0, 6.0, ((0, 4),))
    gain_first = jnp.clip(1.0 + 0.18 * jax.random.normal(seeds[1], (D,), jnp.float32), 0.1, 1.9)
    gain_second = jnp.clip(1.0 + 0.18 * jax.random.normal(seeds[2], (D,), jnp.float32), 0.1, 1.9)
    gate_first = scatter_about(seeds[3], (D, FF), D ** -0.5, 0.109375, ((0, 8), (1, 4)), jnp.float32)
    up_first = scatter_about(seeds[4], (D, FF), D ** -0.5, 0.109375, ((0, 8), (1, 4)), jnp.float32)
    down_first = bell_draw_with(seeds[5], (FF, D), FF ** -0.5, 0.09375, ((0, 8), (1, 4)), (0, 1, 8, 2.0), jnp.float32)
    gate_second = scatter_about(seeds[6], (D, FF), D ** -0.5, 0.109375, ((0, 8), (1, 4)), jnp.float32)
    up_second = scatter_about(seeds[7], (D, FF), D ** -0.5, 0.109375, ((0, 8), (1, 4)), jnp.float32)
    down_second = bell_draw_with(seeds[8], (FF, D), FF ** -0.5, 0.09375, ((0, 8), (1, 4)), (0, 1, 8, 2.0), jnp.float32)
    return {"tokens": tokens, "gain_first": gain_first, "gain_second": gain_second, "gate_first": gate_first, "up_first": up_first, "down_first": down_first, "gate_second": gate_second, "up_second": up_second, "down_second": down_second}


def plain_norm(values):
    values = values.astype(jnp.float32)
    center = lax.optimization_barrier(jnp.mean(values, axis=-1, keepdims=True))
    spread = lax.optimization_barrier(jnp.mean(jnp.square(values - center), axis=-1, keepdims=True))
    return (values - center) * jax.lax.rsqrt(spread + 1e-05)

def fold_gain(weight, scales):
    return (scales[:, None] * weight).astype(jnp.bfloat16)

def half_step(normed, scales, w_gate, w_rising, w_down):
    gate_part = jnp.dot(normed, w_gate, preferred_element_type=jnp.float32)
    rising = jnp.dot(normed, w_rising, preferred_element_type=jnp.float32)
    hidden = (jax.nn.silu(gate_part) * rising).astype(jnp.bfloat16)
    block = jnp.dot(hidden, w_down, preferred_element_type=jnp.float32)
    mixed = 1.6817928 * scales[None, :] * normed.astype(jnp.float32) + 0.5 * block
    return plain_norm(mixed).astype(jnp.bfloat16)

def reference(tokens, gain_first, gain_second, gate_first, up_first, down_first, gate_second, up_second, down_second):
    serve_gate_first = fold_gain(gate_first, gain_first)
    serve_up_first = fold_gain(up_first, gain_first)
    serve_gate_second = fold_gain(gate_second, gain_second)
    serve_up_second = fold_gain(up_second, gain_second)
    serve_down_first = down_first.astype(jnp.bfloat16)
    serve_down_second = down_second.astype(jnp.bfloat16)
    normed_zero = plain_norm(tokens).astype(jnp.bfloat16)
    normed_one = half_step(normed_zero, gain_first, serve_gate_first, serve_up_first, serve_down_first)
    result_rows = half_step(normed_one, gain_second, serve_gate_second, serve_up_second, serve_down_second)
    return (result_rows, serve_gate_first, serve_up_first, serve_down_first, serve_gate_second, serve_up_second, serve_down_second)
```

```python
import jax
import jax.numpy as jnp
from jax import lax
from jax.sharding import PartitionSpec as P


def plain_norm(values):
    values = values.astype(jnp.float32)
    center = jnp.mean(values, axis=-1, keepdims=True)
    spread = jnp.mean(jnp.square(values - center), axis=-1, keepdims=True)
    return (values - center) * lax.rsqrt(spread + 1e-05)


def sum_over_hidden(partial_value):
    pieces = lax.all_to_all(
        partial_value.astype(jnp.bfloat16), "fs", split_axis=1, concat_axis=0, tiled=True
    )
    rows = partial_value.shape[0]
    pieces = pieces.reshape(-1, rows, pieces.shape[1]).astype(jnp.float32)
    summed = jnp.sum(pieces, axis=0).astype(jnp.bfloat16)
    return lax.all_gather(summed, "fs", axis=1, tiled=True).astype(jnp.float32)


def regroup(folded):
    spread = lax.all_to_all(folded, "tp", split_axis=0, concat_axis=1, tiled=True)
    parts = lax.axis_size("fs")
    rows = spread.shape[0]
    owned = lax.all_to_all(spread, "fs", split_axis=1, concat_axis=0, tiled=True)
    owned = owned.reshape(parts, rows, owned.shape[1])
    whole = lax.all_gather(owned, "tp", axis=1, tiled=True)
    return whole.reshape(-1, whole.shape[2])


def half_step(normed, scales, w_gate, w_rising, w_down):
    gate_part = jnp.dot(normed, w_gate, preferred_element_type=jnp.float32)
    rising = jnp.dot(normed, w_rising, preferred_element_type=jnp.float32)
    hidden = (jax.nn.silu(gate_part) * rising).astype(jnp.bfloat16)
    partial_value = jnp.dot(hidden, w_down, preferred_element_type=jnp.float32)
    block = sum_over_hidden(partial_value)
    mixed = 1.6817928 * scales[None, :] * normed.astype(jnp.float32) + 0.5 * block
    return plain_norm(mixed).astype(jnp.bfloat16)


def on_device(
    tokens,
    gain_first,
    gain_second,
    gate_first,
    up_first,
    down_first,
    gate_second,
    up_second,
    down_second,
):
    row_count = gate_first.shape[0]
    offset = lax.axis_index("fs") * row_count

    def fold_gain(weight, scales):
        picked = lax.dynamic_slice_in_dim(scales, offset, row_count, 0)
        return (picked[:, None] * weight).astype(jnp.bfloat16)

    serve_gate_first = regroup(fold_gain(gate_first, gain_first))
    serve_up_first = regroup(fold_gain(up_first, gain_first))
    serve_down_first = lax.all_gather(
        down_first.astype(jnp.bfloat16), "tp", axis=1, tiled=True
    )
    serve_gate_second = regroup(fold_gain(gate_second, gain_second))
    serve_up_second = regroup(fold_gain(up_second, gain_second))
    serve_down_second = lax.all_gather(
        down_second.astype(jnp.bfloat16), "tp", axis=1, tiled=True
    )
    normed_zero = plain_norm(tokens).astype(jnp.bfloat16)
    normed_one = half_step(
        normed_zero, gain_first, serve_gate_first, serve_up_first, serve_down_first
    )
    result_rows = half_step(
        normed_one, gain_second, serve_gate_second, serve_up_second, serve_down_second
    )
    return (
        result_rows,
        serve_gate_first,
        serve_up_first,
        serve_down_first,
        serve_gate_second,
        serve_up_second,
        serve_down_second,
    )


def solution(mesh):
    placed = (
        P("tp", None),
        P(),
        P(),
        P("fs", "tp"),
        P("fs", "tp"),
        P("fs", "tp"),
        P("fs", "tp"),
        P("fs", "tp"),
        P("fs", "tp"),
    )
    return jax.shard_map(
        on_device,
        mesh=mesh,
        in_specs=placed,
        out_specs=(
            P("tp", None),
            P(None, "fs"),
            P(None, "fs"),
            P("fs", None),
            P(None, "fs"),
            P(None, "fs"),
            P("fs", None),
        ),
        check_vma=False,
    )
```

```python
import jax
import jax.numpy as jnp
from jax import lax
from jax.experimental import pallas as pl
from jax.experimental.pallas import tpu as pltpu
from jax.sharding import PartitionSpec as P

import functools

MESH = pl.DeviceIdType.MESH


def can_push(parts, columns, rows, owned):
    return parts == 4 and columns % owned == 0 and owned % 128 == 0 and rows % 128 == 0


def move_kernel(parts, spans, rows, owned, a0, a1, o0, o1, *sems):
    land_s, land_r, x_s, x_r, near_s, near_r, far_s, far_r = sems
    fs = lax.axis_index("fs")
    tp = lax.axis_index("tp")
    plane = tp // 2
    core = tp % 2
    partner = plane * 2 + 1 - core
    across = (1 - plane) * 2 + core
    big = rows * 3 // 8
    small = rows // 8
    sources = (a0, a1)
    results = (o0, o1)

    def piece(is_big, of_core):
        if is_big:
            return of_core * big, big
        return 2 * big + of_core * small, small

    def window(m, origin, span):
        start, length = span
        return results[m].at[pl.ds(pl.multiple_of(origin * rows + start, 16), length), :]

    def copy(src, dst, send, recv, to_fs, to_tp):
        return pltpu.make_async_remote_copy(
            src_ref=src,
            dst_ref=dst,
            send_sem=send,
            recv_sem=recv,
            device_id={"fs": to_fs, "tp": to_tp},
            device_id_type=MESH,
        )

    sends = []
    for m in range(2):
        for k in range(spans):
            shift = lax.rem(fs + k, spans)
            to_fs = tp * spans + shift
            columns = pl.ds(pl.multiple_of(shift * owned, 128), owned)
            for turn in (1, 0):
                for of_core in range(2):
                    to_plane = plane if turn == 0 else 1 - plane
                    to_tp = to_plane * 2 + of_core
                    span = piece(turn == 0, of_core)
                    src = sources[m].at[pl.ds(span[0], span[1]), columns]
                    dst = window(m, fs, span)
                    slot = turn * 2 + of_core
                    sent = copy(src, dst, land_s.at[m, k, slot], land_r.at[m, fs], to_fs, to_tp)
                    if turn == 1:
                        sent.start()
                        sends.append((sent, None))
                    else:
                        same = jnp.logical_and(to_fs == fs, to_tp == tp)
                        pl.when(jnp.logical_not(same))(sent.start)
                        kept = pltpu.make_async_copy(src, dst, land_r.at[m, fs])
                        pl.when(same)(kept.start)
                        sends.append((sent, same))

    def receive(lands_big):
        mine = piece(lands_big, core)
        theirs = piece(not lands_big, core)
        near = piece(lands_big, 1 - core)
        far = piece(not lands_big, 1 - core)

        def to_partner(m, s, span, send, recv):
            part = window(m, s, span)
            return copy(part, part, send.at[m, s], recv.at[m, s], fs, partner)

        def to_across(m, s, span):
            part = window(m, s, span)
            return copy(part, part, x_s.at[m, s], x_r.at[m, s], fs, across)

        for m in range(2):

            @pl.loop(0, parts)
            def _(j, m=m):
                s = lax.rem(fs + j, parts)
                part = window(m, s, mine)
                copy(part, part, x_s.at[m, s], land_r.at[m, s], fs, across).wait_recv()
                to_across(m, s, mine).start()
                to_partner(m, s, mine, near_s, near_r).start()

        for m in range(2):

            @pl.loop(0, parts)
            def _(j, m=m):
                s = lax.rem(fs + j, parts)
                to_across(m, s, theirs).wait_recv()
                to_partner(m, s, theirs, far_s, far_r).start()

        for m in range(2):

            @pl.loop(0, parts)
            def _(j, m=m):
                s = lax.rem(fs + j, parts)
                to_partner(m, s, near, near_s, near_r).wait_recv()
                to_partner(m, s, far, far_s, far_r).wait_recv()
                to_across(m, s, mine).wait_send()
                to_partner(m, s, mine, near_s, near_r).wait_send()
                to_partner(m, s, theirs, far_s, far_r).wait_send()

    own = (fs // spans) // 2 == plane
    pl.when(own)(functools.partial(receive, True))
    pl.when(jnp.logical_not(own))(functools.partial(receive, False))

    for sent, same in sends:
        if same is None:
            sent.wait_send()
        else:
            pl.when(jnp.logical_not(same))(sent.wait_send)


def move(first, second):
    parts = lax.axis_size("fs")
    rows, columns = first.shape
    owned = columns * lax.axis_size("tp") // parts
    spans = columns // owned if columns % owned == 0 else 0
    if not can_push(lax.axis_size("tp"), columns, rows, owned):
        return regroup(first), regroup(second)
    shape = jax.ShapeDtypeStruct((rows * parts, owned), first.dtype)
    per_source = pltpu.SemaphoreType.DMA((2, parts))
    moved = 2 * rows * parts * owned * 2
    return pl.pallas_call(
        functools.partial(move_kernel, parts, spans, rows, owned),
        out_shape=(shape, shape),
        in_specs=[pl.BlockSpec(memory_space=pl.ANY)] * 2,
        out_specs=(pl.BlockSpec(memory_space=pl.ANY),) * 2,
        scratch_shapes=[pltpu.SemaphoreType.DMA((2, spans, 4))] + [per_source] * 7,
        compiler_params=pltpu.CompilerParams(has_side_effects=True),
        cost_estimate=pl.CostEstimate(
            flops=0, bytes_accessed=16 * moved, transcendentals=0
        ),
        name="move_blocks",
    )(first, second)


def plain_norm(values):
    values = values.astype(jnp.float32)
    center = jnp.mean(values, axis=-1, keepdims=True)
    spread = jnp.mean(jnp.square(values - center), axis=-1, keepdims=True)
    return (values - center) * lax.rsqrt(spread + 1e-05)


def sum_over_hidden(partial_value):
    pieces = lax.all_to_all(
        partial_value.astype(jnp.bfloat16), "fs", split_axis=1, concat_axis=0, tiled=True
    )
    rows = partial_value.shape[0]
    pieces = pieces.reshape(-1, rows, pieces.shape[1]).astype(jnp.float32)
    summed = jnp.sum(pieces, axis=0).astype(jnp.bfloat16)
    return lax.all_gather(summed, "fs", axis=1, tiled=True).astype(jnp.float32)


def regroup(folded):
    spread = lax.all_to_all(folded, "tp", split_axis=0, concat_axis=1, tiled=True)
    parts = lax.axis_size("fs")
    rows = spread.shape[0]
    owned = lax.all_to_all(spread, "fs", split_axis=1, concat_axis=0, tiled=True)
    owned = owned.reshape(parts, rows, owned.shape[1])
    whole = lax.all_gather(owned, "tp", axis=1, tiled=True)
    return whole.reshape(-1, whole.shape[2])


def hidden_part(normed, w_gate, w_rising, w_down):
    gate_part = jnp.dot(normed, w_gate, preferred_element_type=jnp.float32)
    rising = jnp.dot(normed, w_rising, preferred_element_type=jnp.float32)
    hidden = (jax.nn.silu(gate_part) * rising).astype(jnp.bfloat16)
    return jnp.dot(hidden, w_down, preferred_element_type=jnp.float32)


def finish(normed, scales, block):
    mixed = 1.6817928 * scales[None, :] * normed.astype(jnp.float32) + 0.5 * block
    return plain_norm(mixed).astype(jnp.bfloat16)


def on_device(
    tokens,
    gain_first,
    gain_second,
    gate_first,
    up_first,
    down_first,
    gate_second,
    up_second,
    down_second,
):
    row_count = gate_first.shape[0]
    offset = lax.axis_index("fs") * row_count

    def fold_gain(weight, scales):
        picked = lax.dynamic_slice_in_dim(scales, offset, row_count, 0)
        return (picked[:, None] * weight).astype(jnp.bfloat16)

    serve_gate_first, serve_up_first = move(
        fold_gain(gate_first, gain_first), fold_gain(up_first, gain_first)
    )
    serve_down_first = lax.all_gather(
        down_first.astype(jnp.bfloat16), "tp", axis=1, tiled=True
    )
    normed_zero = plain_norm(tokens).astype(jnp.bfloat16)
    partial_first = hidden_part(
        normed_zero, serve_gate_first, serve_up_first, serve_down_first
    )
    partial_first, gate_folded, up_folded = lax.optimization_barrier(
        (partial_first, fold_gain(gate_second, gain_second), fold_gain(up_second, gain_second))
    )
    serve_gate_second, serve_up_second = move(gate_folded, up_folded)
    serve_down_second = lax.all_gather(
        down_second.astype(jnp.bfloat16), "tp", axis=1, tiled=True
    )
    block_first = lax.psum(partial_first, "fs")
    normed_one = finish(normed_zero, gain_first, block_first)
    partial_second = hidden_part(
        normed_one, serve_gate_second, serve_up_second, serve_down_second
    )
    result_rows = finish(normed_one, gain_second, sum_over_hidden(partial_second))
    return (
        result_rows,
        serve_gate_first,
        serve_up_first,
        serve_down_first,
        serve_gate_second,
        serve_up_second,
        serve_down_second,
    )


def solution(mesh):
    placed = (
        P("tp", None),
        P(),
        P(),
        P("fs", "tp"),
        P("fs", "tp"),
        P("fs", "tp"),
        P("fs", "tp"),
        P("fs", "tp"),
        P("fs", "tp"),
    )
    return jax.shard_map(
        on_device,
        mesh=mesh,
        in_specs=placed,
        out_specs=(
            P("tp", None),
            P(None, "fs"),
            P(None, "fs"),
            P("fs", None),
            P(None, "fs"),
            P(None, "fs"),
            P("fs", None),
        ),
        check_vma=False,
    )
```

```python
import jax
import jax.numpy as jnp
from jax import lax
from jax.experimental import pallas as pl
from jax.experimental.pallas import tpu as pltpu
from jax.sharding import PartitionSpec as P

import functools

MESH = pl.DeviceIdType.MESH


def can_push(members, parts, columns, rows):
    blocks = parts // members
    if parts % members or columns % (blocks * 128):
        return False
    return rows % (members * 16) == 0


def scatter_kernel(parts, members, source, result, send_sems, recv_sems):
    fs = lax.axis_index("fs")
    tp = lax.axis_index("tp")
    blocks = parts // members
    rows = source.shape[0] // members
    owned = source.shape[1] // blocks
    landing = result.at[pl.ds(pl.multiple_of(fs * rows, 16), rows), :]

    sends = []
    for k in range(blocks):
        block = lax.rem(fs + k, blocks)
        to_fs = tp * blocks + block
        columns = pl.ds(pl.multiple_of(block * owned, 128), owned)
        for q in range(members):
            to_tp = lax.rem(tp + q, members)
            src = source.at[pl.ds(pl.multiple_of(to_tp * rows, 16), rows), columns]
            sent = pltpu.make_async_remote_copy(
                src_ref=src,
                dst_ref=landing,
                send_sem=send_sems.at[k, q],
                recv_sem=recv_sems.at[fs],
                device_id={"fs": to_fs, "tp": to_tp},
                device_id_type=MESH,
            )
            if q:
                sent.start()
                sends.append((sent, None))
                continue
            same = to_fs == fs
            pl.when(jnp.logical_not(same))(sent.start)
            pl.when(same)(pltpu.make_async_copy(src, landing, recv_sems.at[fs]).start)
            sends.append((sent, same))

    for s in range(parts):
        part = result.at[pl.ds(s * rows, rows), :]
        pltpu.make_async_remote_copy(
            src_ref=part,
            dst_ref=part,
            send_sem=send_sems.at[0, 0],
            recv_sem=recv_sems.at[s],
            device_id={"fs": fs, "tp": lax.rem(tp + 1, members)},
            device_id_type=MESH,
        ).wait_recv()

    for sent, same in sends:
        if same is None:
            sent.wait_send()
        else:
            pl.when(jnp.logical_not(same))(sent.wait_send)


def scatter(folded):
    parts = lax.axis_size("fs")
    members = lax.axis_size("tp")
    rows, columns = folded.shape
    blocks = parts // members
    shape = (parts * rows // members, columns // blocks)
    moved = 2 * shape[0] * shape[1]
    return pl.pallas_call(
        functools.partial(scatter_kernel, parts, members),
        out_shape=jax.ShapeDtypeStruct(shape, folded.dtype),
        in_specs=[pl.BlockSpec(memory_space=pl.ANY)],
        out_specs=pl.BlockSpec(memory_space=pl.ANY),
        scratch_shapes=[
            pltpu.SemaphoreType.DMA((blocks, members)),
            pltpu.SemaphoreType.DMA((parts,)),
        ],
        compiler_params=pltpu.CompilerParams(has_side_effects=True),
        cost_estimate=pl.CostEstimate(
            flops=0, bytes_accessed=64 * moved, transcendentals=0
        ),
        name="scatter_pieces",
    )(folded)


def widen(pieces):
    return ordered(lax.all_gather(pieces, "tp", axis=0))


def ordered(gathered):
    parts = lax.axis_size("fs")
    members, rows, owned = gathered.shape
    split = gathered.reshape(members, parts, rows // parts, owned)
    return split.transpose(1, 0, 2, 3).reshape(members * rows, owned)


def plain_norm(values):
    values = values.astype(jnp.float32)
    center = jnp.mean(values, axis=-1, keepdims=True)
    spread = jnp.mean(jnp.square(values - center), axis=-1, keepdims=True)
    return (values - center) * lax.rsqrt(spread + 1e-05)


def sum_over_hidden(partial_value):
    pieces = lax.all_to_all(
        partial_value.astype(jnp.bfloat16), "fs", split_axis=1, concat_axis=0, tiled=True
    )
    rows = partial_value.shape[0]
    pieces = pieces.reshape(-1, rows, pieces.shape[1]).astype(jnp.float32)
    summed = jnp.sum(pieces, axis=0).astype(jnp.bfloat16)
    return lax.all_gather(summed, "fs", axis=1, tiled=True).astype(jnp.float32)


def regroup(folded):
    spread = lax.all_to_all(folded, "tp", split_axis=0, concat_axis=1, tiled=True)
    parts = lax.axis_size("fs")
    rows = spread.shape[0]
    owned = lax.all_to_all(spread, "fs", split_axis=1, concat_axis=0, tiled=True)
    owned = owned.reshape(parts, rows, owned.shape[1])
    whole = lax.all_gather(owned, "tp", axis=1, tiled=True)
    return whole.reshape(-1, whole.shape[2])


def hidden_part(normed, w_gate, w_rising, w_down):
    gate_part = jnp.dot(normed, w_gate, preferred_element_type=jnp.float32)
    rising = jnp.dot(normed, w_rising, preferred_element_type=jnp.float32)
    hidden = (jax.nn.silu(gate_part) * rising).astype(jnp.bfloat16)
    return jnp.dot(hidden, w_down, preferred_element_type=jnp.float32)


def finish(normed, scales, block):
    mixed = 1.6817928 * scales[None, :] * normed.astype(jnp.float32) + 0.5 * block
    return plain_norm(mixed).astype(jnp.bfloat16)


def on_device(
    tokens,
    gain_first,
    gain_second,
    gate_first,
    up_first,
    down_first,
    gate_second,
    up_second,
    down_second,
):
    row_count = gate_first.shape[0]
    offset = lax.axis_index("fs") * row_count

    def fold_gain(weight, scales):
        picked = lax.dynamic_slice_in_dim(scales, offset, row_count, 0)
        return (picked[:, None] * weight).astype(jnp.bfloat16)

    folded = (
        fold_gain(gate_first, gain_first),
        fold_gain(up_first, gain_first),
        fold_gain(gate_second, gain_second),
        fold_gain(up_second, gain_second),
    )
    down_rounded, scattered_first = lax.optimization_barrier(
        (down_first.astype(jnp.bfloat16), folded[0])
    )
    folded = (scattered_first,) + folded[1:]
    serve_down_first = lax.all_gather(down_rounded, "tp", axis=1, tiled=True)
    serve_down_second = lax.all_gather(
        down_second.astype(jnp.bfloat16), "tp", axis=1, tiled=True
    )
    normed_zero = plain_norm(tokens).astype(jnp.bfloat16)
    members = lax.axis_size("tp")
    if can_push(members, lax.axis_size("fs"), gate_first.shape[1], row_count):
        pieces = [scatter(folded[0])]
        for weight in folded[1:]:
            weight, pieces[-1] = lax.optimization_barrier((weight, pieces[-1]))
            pieces.append(scatter(weight))
        normed_zero, pieces[3] = lax.optimization_barrier((normed_zero, pieces[3]))
        served = [widen(piece) for piece in pieces[:2]]
        later = [lax.all_gather(piece, "tp", axis=0) for piece in pieces[2:]]
    else:
        served = [regroup(weight) for weight in folded]
        later = []
    serve_gate_first, serve_up_first = served[:2]
    partial_first = hidden_part(
        normed_zero, serve_gate_first, serve_up_first, serve_down_first
    )
    normed_one = finish(normed_zero, gain_first, sum_over_hidden(partial_first))
    if later:
        normed_one, *later = lax.optimization_barrier((normed_one, *later))
        served += [ordered(gathered) for gathered in later]
    serve_gate_second, serve_up_second = served[2:]
    partial_second = hidden_part(
        normed_one, serve_gate_second, serve_up_second, serve_down_second
    )
    result_rows = finish(normed_one, gain_second, sum_over_hidden(partial_second))
    return (
        result_rows,
        serve_gate_first,
        serve_up_first,
        serve_down_first,
        serve_gate_second,
        serve_up_second,
        serve_down_second,
    )


def solution(mesh):
    placed = (
        P("tp", None),
        P(),
        P(),
        P("fs", "tp"),
        P("fs", "tp"),
        P("fs", "tp"),
        P("fs", "tp"),
        P("fs", "tp"),
        P("fs", "tp"),
    )
    return jax.shard_map(
        on_device,
        mesh=mesh,
        in_specs=placed,
        out_specs=(
            P("tp", None),
            P(None, "fs"),
            P(None, "fs"),
            P("fs", None),
            P(None, "fs"),
            P(None, "fs"),
            P("fs", None),
        ),
        check_vma=False,
    )
```
